512 devices in a mesh: sp: 16 (over z), fs: 4 (over y), tp: 8 (over x, core).
Axes of the slice: x: 4, y: 4, z: 16, core: 2. Of those that a mesh axis runs over, the one named last changes fastest.
Arguments:
- tokens: bfloat16 [4, 4096, 2048], P('fs', 'sp'), may hold values from -6 to 6
- norm_gain: float32 [2048], replicated, may hold values from 0.1 to 1.9
- pool_input: bfloat16 [2048, 2048], P(('sp', 'fs'), 'tp'), may hold values from -0.125 to 0.125
- query_weight: bfloat16 [2048, 2048], P(('sp', 'fs'), 'tp'), may hold values from -20 to 20
- key_weight: bfloat16 [2048, 2048], P(('sp', 'fs'), 'tp'), may hold values from -1 to 1
- value_weight: bfloat16 [2048, 2048], P(('sp', 'fs'), 'tp'), may hold values from -0.125 to 0.125
- pool_map: bfloat16 [8, 256, 256], P('tp'), may hold values from -0.375 to 0.375
- pool_scale: float32 [2048], P('tp'), may hold values from 0.1 to 1.9
- head_gain: float32 [256], replicated, may hold values from 0.1 to 1.9
- diff_lambda: float32 [8], replicated, may hold values from 0.3 to 0.8
- out_pool: bfloat16 [2048, 2048], P('tp', ('sp', 'fs')), may hold values from -0.09375 to 0.09375
- out_heads: bfloat16 [2048, 2048], P('tp', ('sp', 'fs')), may hold values from -0.09375 to 0.09375
Outputs:
- layer_out: bfloat16 [4, 4096, 2048], P('fs', 'sp', 'tp')
The draws below stay inside these ranges and needn't reach their ends.
All inputs are finite; a program needn't handle non-finite values.
Results may differ from the reference program's by a relative error of at most 0.018.
Values may be sent and summed in bfloat16 or wider, within the bound.
A program may use at most 64 MiB of HBM per device.

```python
import math
import jax
import jax.numpy as jnp
from jax import lax

D = 2048
HEADS = 8
HEAD_DIM = 128
POOL_GROUPS = 8
GROUP_DIM = 256
POOL_WIDTH = 2048
SEQ = 4096
SEQS = 4
N_TP = 8


def key_matrix(key):
    normal_part = jax.random.truncated_normal(jax.random.fold_in(key, 11), -6.0, 6.0, (D, 2 * HEADS * HEAD_DIM), jnp.float32)
    return normal_part * D ** (-0.5)


def draw_key_weight(key, part):
    return key_matrix(key).astype(jnp.bfloat16)


def draw_query_weight(key, part):
    normal_part = jax.random.truncated_normal(jax.random.fold_in(key, 12), -6.0, 6.0, (D, 2 * HEADS * HEAD_DIM), jnp.float32)
    result = normal_part * (3.0 / D) ** 0.5
    return result.astype(jnp.bfloat16)


def levels(key, shape, cuts, smallest, high):
    loudness, own = 1.0, jax.random.fold_in(key, 6)
    for dim, shards_of in cuts:
        draws = jnp.exp(jax.random.uniform(jax.random.fold_in(own, dim), (shards_of,), jnp.float32, smallest / len(cuts), high / len(cuts)))
        loudness = loudness * jnp.repeat(draws, shape[dim] // shards_of).reshape([-1 if axis == dim else 1 for axis in range(len(shape))])
    return loudness


def normal_values(key, extent, spread, limit, split=(), kind=jnp.bfloat16):
    array = jax.random.normal(key, extent, jnp.float32) * spread
    if len(split) > 0:
        array = levels(key, extent, split, -0.22, 0.18) * array
    return jnp.clip(array, min=-limit, max=limit).astype(kind)


def setup_inputs(seed: int = 0) -> dict:
    arg_keys = jax.random.split(jax.random.key(seed), 13)
    return {
        "tokens": normal_values(arg_keys[0], (SEQS, SEQ, D), 1.0, 6.0, ((0, 4), (1, 16))),
        "norm_gain": jnp.clip(1.0 + 0.18 * jax.random.normal(arg_keys[1], (D,), jnp.float32), 0.1, 1.9),
        "pool_input": normal_values(arg_keys[2], (D, POOL_WIDTH), D ** -0.5, 0.125, ((0, 64), (1, 8))),
        "query_weight": draw_query_weight(jax.random.fold_in(arg_keys[12], 71), 0),
        "key_weight": draw_key_weight(jax.random.fold_in(arg_keys[12], 71), 0),
        "value_weight": normal_values(arg_keys[5], (D, 2 * HEADS * HEAD_DIM), D ** -0.5, 0.125, ((0, 64), (1, 8))),
        "pool_map": normal_values(arg_keys[6], (POOL_GROUPS, GROUP_DIM, GROUP_DIM), GROUP_DIM ** -0.5, 0.375, ((0, 8),)),
        "pool_scale": jnp.clip(1.0 + 0.18 * jax.random.normal(arg_keys[7], (POOL_WIDTH,), jnp.float32), 0.1, 1.9),
        "head_gain": jnp.clip(1.0 + 0.18 * jax.random.normal(arg_keys[8], (2 * HEAD_DIM,), jnp.float32), 0.1, 1.9),
        "diff_lambda": jnp.clip(jax.random.uniform(arg_keys[9], (HEADS,), jnp.float32, 0.3, 0.8), 0.3, 0.8),
        "out_pool": normal_values(arg_keys[10], (POOL_WIDTH, D), (POOL_WIDTH + 2 * HEADS * HEAD_DIM) ** -0.5, 0.09375, ((0, 8), (1, 64))),
        "out_heads": normal_values(arg_keys[11], (2 * HEADS * HEAD_DIM, D), (POOL_WIDTH + 2 * HEADS * HEAD_DIM) ** -0.5, 0.09375, ((0, 8), (1, 64))),
    }


THETA = 500000.0
HEAD_SCALE = 0.8
NORM_EPS = 1e-06
HEAD_EPS = 1e-05

def rotate(tensor, positions):
    half = HEAD_DIM // 2
    freqs = 1.0 / THETA ** (jnp.arange(half, dtype=jnp.float32) * 2.0 / HEAD_DIM)
    angles = positions[:, None] * freqs[None, :]
    cosine = jnp.cos(angles)[:, None, None, :]
    sine = jnp.sin(angles)[:, None, None, :]
    floated = tensor.astype(jnp.float32)
    first = floated[..., :half]
    second = floated[..., half:]
    turned = jnp.concatenate([first * cosine - second * sine, second * cosine + first * sine], -1)
    return turned.astype(jnp.bfloat16)

def one_sequence(seq_tokens, norm_gain, pool_input, query_weight, key_weight, value_weight, pool_map, pool_scale, head_gain, diff_lambda, out_pool, out_heads):
    length = seq_tokens.shape[0]
    floated = seq_tokens.astype(jnp.float32)
    normed = (floated * lax.rsqrt(lax.optimization_barrier(jnp.mean(floated * floated, -1, keepdims=True)) + NORM_EPS) * norm_gain).astype(jnp.bfloat16)
    pool_in = jnp.dot(normed, pool_input, preferred_element_type=jnp.float32).astype(jnp.bfloat16)
    queries = jnp.dot(normed, query_weight, preferred_element_type=jnp.float32).astype(jnp.bfloat16)
    keys_all = jnp.dot(normed, key_weight, preferred_element_type=jnp.float32).astype(jnp.bfloat16)
    values = jnp.dot(normed, value_weight, preferred_element_type=jnp.float32).astype(jnp.bfloat16)
    positions = jnp.arange(length, dtype=jnp.float32)
    queries = rotate(queries.reshape(length, HEADS, 2, HEAD_DIM), positions)
    keys_all = rotate(keys_all.reshape(length, HEADS, 2, HEAD_DIM), positions)
    values = values.reshape(length, HEADS, 2 * HEAD_DIM)
    span = math.gcd(length, 512)

    def one_head(operands):
        query_head, key_head, value_head, lambda_head = operands
        key_float = key_head.astype(jnp.float32)
        value_float = value_head.astype(jnp.float32)

        def one_block(begin):
            query_block = lax.dynamic_slice_in_dim(query_head, begin, span, 0).astype(jnp.float32)
            scores = jnp.einsum('qcd,kcd->cqk', query_block, key_float) * HEAD_DIM ** (-0.5)
            query_pos = begin + jnp.arange(span, dtype=jnp.int32)
            key_pos = jnp.arange(length, dtype=jnp.int32)
            scores = jnp.where(query_pos[:, None] >= key_pos[None, :], scores, -jnp.inf)
            largest = lax.optimization_barrier(jnp.max(scores, -1, keepdims=True))
            expons = jnp.exp(scores - largest)
            totals = lax.optimization_barrier(jnp.sum(expons, -1))
            expons_low = expons.astype(jnp.bfloat16).astype(jnp.float32)
            map_values = jnp.einsum('cqk,ke->cqe', expons_low, value_float)
            return map_values[0] / totals[0][:, None] - lambda_head * map_values[1] / totals[1][:, None]
        begins = jnp.arange(length // span, dtype=jnp.int32) * span
        return lax.map(one_block, begins).reshape(length, 2 * HEAD_DIM)
    heads_raw = lax.map(one_head, (jnp.moveaxis(queries, 1, 0), jnp.moveaxis(keys_all, 1, 0), jnp.moveaxis(values, 1, 0), diff_lambda))
    heads_raw = jnp.moveaxis(heads_raw, 0, 1)
    attn = (heads_raw * lax.rsqrt(lax.optimization_barrier(jnp.mean(heads_raw * heads_raw, -1, keepdims=True)) + HEAD_EPS) * head_gain * HEAD_SCALE).astype(jnp.bfloat16).reshape(length, 2 * HEADS * HEAD_DIM)
    grouped = pool_in.reshape(length, POOL_GROUPS, GROUP_DIM).astype(jnp.float32)
    running = jnp.concatenate([jnp.zeros((1, POOL_GROUPS, GROUP_DIM), jnp.float32), jnp.cumsum(grouped, 0)], 0)
    windows = 2 ** (1 + jnp.arange(POOL_GROUPS, dtype=jnp.int32) % 4)
    places = jnp.arange(length, dtype=jnp.int32)[:, None]
    lowest = jnp.maximum(places + 1 - windows[None, :], 0)
    counts = jnp.minimum(places + 1, windows[None, :]).astype(jnp.float32)
    low_sums = running[lowest, jnp.arange(POOL_GROUPS, dtype=jnp.int32)[None, :]]
    window_mean = (running[1:] - low_sums) / counts[:, :, None]
    pool_mixed = (window_mean - grouped).astype(jnp.bfloat16)
    pooled = (jnp.einsum('sgc,gce->sge', pool_mixed.astype(jnp.float32), pool_map.astype(jnp.float32)) * pool_scale.reshape(POOL_GROUPS, GROUP_DIM)).astype(jnp.bfloat16).reshape(length, POOL_WIDTH)
    pool_cols = POOL_WIDTH // N_TP
    head_cols = 2 * HEADS * HEAD_DIM // N_TP
    summed = jnp.zeros((length, D), jnp.float32)
    for shard_index in range(N_TP):
        pool_part = pooled[:, shard_index * pool_cols:(shard_index + 1) * pool_cols]
        head_part = attn[:, shard_index * head_cols:(shard_index + 1) * head_cols]
        partial_value = jnp.dot(pool_part, out_pool[shard_index * pool_cols:(shard_index + 1) * pool_cols], preferred_element_type=jnp.float32) + jnp.dot(head_part, out_heads[shard_index * head_cols:(shard_index + 1) * head_cols], preferred_element_type=jnp.float32)
        rounded = lax.optimization_barrier(partial_value.astype(jnp.bfloat16))
        summed = summed + rounded.astype(jnp.float32)
    return summed.astype(jnp.bfloat16)

def reference(tokens, norm_gain, pool_input, query_weight, key_weight, value_weight, pool_map, pool_scale, head_gain, diff_lambda, out_pool, out_heads):

    def apply_one(seq_tokens):
        return one_sequence(seq_tokens, norm_gain, pool_input, query_weight, key_weight, value_weight, pool_map, pool_scale, head_gain, diff_lambda, out_pool, out_heads)
    return lax.map(apply_one, tokens)
```

```python
import functools

import numpy as np
import jax
import jax.numpy as jnp
from jax import lax
from jax.experimental import pallas as pl
from jax.experimental.pallas import tpu as pltpu
from jax.sharding import PartitionSpec as P

HEAD_DIM = 128
THETA = 500000.0
HEAD_SCALE = 0.8
NORM_EPS = 1e-06
HEAD_EPS = 1e-05
NEG = -1e30
F32 = jnp.float32
BF16 = jnp.bfloat16
MESH = pl.DeviceIdType.MESH
LOG2E = 1.4426950408889634


def rope_tables(rows, blocks):
    half = HEAD_DIM // 2
    freqs = 1.0 / THETA ** (np.arange(half, dtype=np.float64) * 2.0 / HEAD_DIM)
    tables = []
    for offsets in (np.arange(rows), np.arange(blocks) * rows):
        angles = offsets[:, None] * freqs[None, :]
        cosine, sine = np.cos(angles), np.sin(angles)
        tables.append(np.concatenate([cosine, cosine], 1).astype(np.float32))
        tables.append(np.concatenate([sine, sine], 1).astype(np.float32))
    return tables


def remote(src, dst, send, recv, **where):
    return pltpu.make_async_remote_copy(
        src_ref=src, dst_ref=dst, send_sem=send, recv_sem=recv, device_id=where, device_id_type=MESH
    )


def nt_dot(a, b):
    return lax.dot_general(a, b, (((1,), (1,)), ((), ())), preferred_element_type=F32)


def kernel(
    nz, ny, nt,
    tok, gain, pin, qw, kw, vw, pmap, pscale, hgain, lam, opool, ohead,
    rowcos, rowsin, blkcos, blksin,
    out,
    nrm, wkv, wqp, wo, kv, qbuf, poolbuf, rim, bra, part, rs,
    m_ref, l_ref, acc,
    loc_sem, zsend, zrecv, ysend, yleft, yright, yopp, ksend, krecv, rimsem, rssend, rsrecv,
):
    z = lax.axis_index("sp")
    y = lax.axis_index("fs")
    t = lax.axis_index("tp")
    zr1 = lax.rem(z + 1, nz)
    zl1 = lax.rem(z + nz - 1, nz)
    yr1 = lax.rem(y + 1, ny)
    yl1 = lax.rem(y + ny - 1, ny)
    rows = tok.shape[0]
    far = nz // 2
    groups = (wkv, wqp, wo)

    def slot(zz, yy):
        return pl.ds(pl.multiple_of(zz * 128 + yy * 32, 32), 32)

    own = slot(z, y)
    loads = [
        pltpu.make_async_copy(kw, wkv.at[own, 0:256], loc_sem.at[0]),
        pltpu.make_async_copy(vw, wkv.at[own, 256:512], loc_sem.at[1]),
        pltpu.make_async_copy(pin, wqp.at[own, 0:256], loc_sem.at[2]),
        pltpu.make_async_copy(qw, wqp.at[own, 256:512], loc_sem.at[3]),
    ]
    for load in loads:
        load.start()

    barrier = pltpu.get_barrier_semaphore()
    for where in ({"sp": zr1}, {"sp": zl1}, {"fs": yr1}, {"fs": yl1}):
        pl.semaphore_signal(barrier, inc=1, device_id=where, device_id_type=MESH)
    for k in range(1, nt):
        pl.semaphore_signal(
            barrier, inc=1, device_id={"tp": lax.rem(t + k, nt)}, device_id_type=MESH
        )
    for load in loads:
        load.wait()
    pl.semaphore_wait(barrier, 4 + nt - 1)

    def zslot(s, way):
        return lax.rem(z + nz - s, nz) if way == 0 else lax.rem(z + s, nz)

    def zcopy(g, way, s):
        at = slot(zslot(s, way), y)
        peer = zr1 if way == 0 else zl1
        return remote(
            groups[g].at[at], groups[g].at[at], zsend.at[g, way, s], zrecv.at[g, way, s], sp=peer
        )

    def zwait(g, way, s):
        at = slot(zslot(s, way), y)
        remote(
            groups[g].at[at], groups[g].at[at], zsend.at[g, way, s - 1], zrecv.at[g, way, s - 1], sp=zl1
        ).wait_recv()

    last = (far, nz - far - 1)

    def index_of(s, way):
        return 0 if s == 0 else 2 * s - 1 + way

    def steps_at(s):
        return [(s, way) for way in (0, 1) if s <= last[way] and not (s == 0 and way == 1)]

    def ysend_slots(g, s, way):
        buf = groups[g]
        at = slot(zslot(s, way), y)
        i = index_of(s, way)
        remote(buf.at[at], buf.at[at], ysend.at[g], yleft.at[g, i], fs=yr1).start()
        remote(buf.at[at], buf.at[at], ysend.at[g], yright.at[g, i], fs=yl1).start()

    def yrelay(g, s, way):
        buf = groups[g]
        zz = zslot(s, way)
        i = index_of(s, way)
        at = slot(zz, yl1)
        remote(buf.at[at], buf.at[at], ysend.at[g], yleft.at[g, i], fs=yr1).wait_recv()
        half = pl.ds(pl.multiple_of(zz * 128 + yl1 * 32, 16), 16)
        remote(buf.at[half], buf.at[half], ysend.at[g], yopp.at[g, 0], fs=yr1).start()
        at = slot(zz, yr1)
        remote(buf.at[at], buf.at[at], ysend.at[g], yright.at[g, i], fs=yl1).wait_recv()
        half = pl.ds(pl.multiple_of(zz * 128 + yr1 * 32 + 16, 16), 16)
        remote(buf.at[half], buf.at[half], ysend.at[g], yopp.at[g, 1], fs=yl1).start()

    def yfinish(g):
        buf = groups[g]
        for way in (0, 1):
            quarter = buf.at[pl.ds(0, nz * 16)]
            remote(quarter, quarter, ysend.at[g], yopp.at[g, way], fs=yr1).wait_recv()

    for g in (0, 1):
        for way in (0, 1):
            zcopy(g, way, 0).start()
    ysend_slots(0, 0, 0)

    eye = (
        lax.broadcasted_iota(jnp.int32, (256, 256), 0) == lax.broadcasted_iota(jnp.int32, (256, 256), 1)
    ).astype(BF16)
    for which, src in ((0, opool), (1, ohead)):
        turned = lax.dot_general(
            src[...], eye, (((0,), (0,)), ((), ())), preferred_element_type=F32
        )
        wo[own, which * 256 : which * 256 + 256] = turned.astype(BF16)

    def norm_rows(i, carry):
        at = pl.ds(pl.multiple_of(i * 32, 32), 32)
        x = tok[at, :].astype(F32)
        scale = lax.rsqrt(jnp.mean(x * x, -1, keepdims=True) + NORM_EPS)
        nrm[at, :] = (x * scale * gain[...]).astype(BF16)
        return carry

    lax.fori_loop(0, rows // 32, norm_rows, 0)
    for way in (0, 1):
        zcopy(2, way, 0).start()

    for s in range(1, far + 1):
        for g in range(3):
            for step, way in steps_at(s):
                zwait(g, way, step)
                if step < last[way]:
                    zcopy(g, way, step).start()
                if g == 0:
                    ysend_slots(0, step, way)
        for step, way in steps_at(s - 1):
            yrelay(0, step, way)
    for step, way in steps_at(far):
        yrelay(0, step, way)
    yfinish(0)

    cosine = rowcos[...] * blkcos[pl.ds(z, 1), :] - rowsin[...] * blksin[pl.ds(z, 1), :]
    sine = rowsin[...] * blkcos[pl.ds(z, 1), :] + rowcos[...] * blksin[pl.ds(z, 1), :]
    first = lax.broadcasted_iota(jnp.int32, sine.shape, 1) < HEAD_DIM // 2
    signed = jnp.where(first, -sine, sine)

    def rotated(x):
        x = x.astype(BF16).astype(F32)
        return (x * cosine + pltpu.roll(x, HEAD_DIM // 2, 1) * signed).astype(BF16)

    home = pl.ds(pl.multiple_of(z * rows, rows), rows)
    product = jnp.dot(nrm[...], wkv[:, 0:256], preferred_element_type=F32)
    kv[home, 0:128] = rotated(product[:, 0:128])
    kv[home, 128:256] = rotated(product[:, 128:256])
    kv[home, 256:512] = jnp.dot(nrm[...], wkv[:, 256:512], preferred_element_type=F32).astype(BF16)

    halfrows = rows // 2

    def kslot(s, way, half):
        zz = lax.rem(z + nz - s, nz) if way == 0 else lax.rem(z + s, nz)
        return pl.ds(pl.multiple_of(zz * rows + half * halfrows, halfrows), halfrows)

    def kcopy(s, way, half):
        at = kslot(s, way, half)
        return remote(
            kv.at[at], kv.at[at], ksend.at[way, s, half], krecv.at[way, s, half],
            sp=zr1 if way == 0 else zl1,
        )

    def kwait(s, way, half):
        at = kslot(s, way, half)
        remote(
            kv.at[at], kv.at[at], ksend.at[way, s - 1, half], krecv.at[way, s - 1, half], sp=zl1
        ).wait_recv()

    for half in (0, 1):
        for way in (0, 1):
            kcopy(0, way, half).start()

    order = [pair for s in range(far + 1) for pair in steps_at(s)]
    for step, way in order:
        ysend_slots(1, step, way)

    def ring(s):
        for half in (0, 1):
            for way in (0, 1):
                if s <= last[way]:
                    kwait(s, way, half)
                    if s < last[way]:
                        kcopy(s, way, half).start()

    for s in (1, 2):
        ring(s)
        for step, way in order[(s - 1) * 8 : s * 8]:
            yrelay(1, step, way)
    for step, way in order:
        ysend_slots(2, step, way)
    ring(3)
    yfinish(1)

    product = jnp.dot(nrm[...], wqp[:, 256:512], preferred_element_type=F32)
    qbuf[:, 0:128] = rotated(product[:, 0:128])
    qbuf[:, 128:256] = rotated(product[:, 128:256])
    poolbuf[...] = jnp.dot(nrm[...], wqp[:, 0:256], preferred_element_type=F32).astype(BF16)
    rimcopy = remote(
        poolbuf.at[pl.ds(rows - 16, 16)], rim, rimsem.at[0], rimsem.at[1], sp=zr1
    )
    rimcopy.start()

    score_scale = HEAD_DIM ** (-0.5) * LOG2E

    def scores_of(j, m):
        at = pl.ds(pl.multiple_of(j * rows, rows), rows)
        cols = pl.ds(m * HEAD_DIM, HEAD_DIM)
        return nt_dot(qbuf[:, cols], kv[at, cols]) * score_scale

    def values_of(j):
        return kv[pl.ds(pl.multiple_of(j * rows, rows), rows), 256:512]

    for m in (0, 1):
        s0 = scores_of(z, m)
        above = lax.broadcasted_iota(jnp.int32, s0.shape, 1) > lax.broadcasted_iota(jnp.int32, s0.shape, 0)
        s0 = jnp.where(above, -jnp.inf, s0)
        top = jnp.max(s0, -1, keepdims=True)
        p = jnp.exp2(s0 - top)
        m_ref[m] = top
        l_ref[m] = jnp.sum(p, -1, keepdims=True)
        acc[m] = jnp.dot(p.astype(BF16), values_of(z), preferred_element_type=F32)

    def attend(j):
        for m in (0, 1):
            s0 = scores_of(j, m)
            old = m_ref[m]
            top = jnp.maximum(old, jnp.max(s0, -1, keepdims=True))
            p = jnp.exp2(s0 - top)
            shrink = jnp.exp2(old - top)
            m_ref[m] = top
            l_ref[m] = l_ref[m] * shrink + jnp.sum(p, -1, keepdims=True)
            acc[m] = acc[m] * shrink + jnp.dot(
                p.astype(BF16), values_of(j), preferred_element_type=F32
            )

    def attend_step(s):
        def one(way, carry):
            j = jnp.where(way == 0, z - s, z + s - nz)

            @pl.when(jnp.logical_and(j >= 0, s + way <= far))
            def _():
                attend(j)

            return carry

        lax.fori_loop(0, 2, one, 0)

    def backlog(s, carry):
        attend_step(s)
        return carry

    lax.fori_loop(1, 4, backlog, 0)

    for s in range(4, far + 1):
        ring(s)
        if s in (5, 6):
            for step, way in order[(s - 5) * 8 : (s - 4) * 8]:
                yrelay(2, step, way)
        if s == 4:
            rimcopy.wait_recv()
            level = lax.rem(t, 4)
            inner = poolbuf[...].astype(F32)
            before = jnp.where(z == 0, 0.0, rim[...].astype(F32))
            grown = jnp.concatenate([before, inner], 0)
            picked = jnp.zeros_like(grown)
            for power in range(4):
                grown = grown + pltpu.roll(grown, 1 << power, 0)
                picked = jnp.where(level == power, grown, picked)
            place = z * rows + lax.broadcasted_iota(jnp.int32, (rows, 1), 0)
            window = jnp.left_shift(2, level)
            count = jnp.minimum(place + 1, window).astype(F32)
            mixed = (picked[16:, :] / count - inner).astype(BF16)
            pooled = jnp.dot(mixed, pmap[0], preferred_element_type=F32) * pscale[...]
            bra[:, 0:256] = pooled.astype(BF16)
        attend_step(s)

    yfinish(2)
    heads = acc[0] / l_ref[0] - lam[t] * (acc[1] / l_ref[1])
    scale = lax.rsqrt(jnp.mean(heads * heads, -1, keepdims=True) + HEAD_EPS)
    bra[:, 256:512] = (heads * scale * hgain[...] * HEAD_SCALE).astype(BF16)

    def partial_of(peer):
        at = pl.ds(pl.multiple_of(peer * 256, 256), 256)
        return nt_dot(bra[...], wo[at, :]).astype(BF16)

    def rcopy(k):
        peer = lax.rem(t + k, nt)
        return remote(part.at[k], rs.at[k], rssend.at[k], rsrecv.at[k], tp=peer)

    def emit(i, carry):
        k = i + 1
        part[k] = partial_of(lax.rem(t + k, nt))
        rcopy(k).start()
        return carry

    lax.fori_loop(0, nt - 1, emit, 0)
    total = partial_of(t).astype(F32)
    for k in range(1, nt):
        rcopy(k).wait_recv()
        total = total + rs[k].astype(F32)
    out[...] = total.astype(BF16)

    for g in range(3):
        for way in (0, 1):
            for s in range(last[way]):
                zcopy(g, way, s).wait_send()
        whole = groups[g].at[pl.ds(0, nz * 96)]
        remote(whole, whole, ysend.at[g], yopp.at[g, 0], fs=yr1).wait_send()
    for way in (0, 1):
        for s in range(last[way]):
            for half in (0, 1):
                kcopy(s, way, half).wait_send()
    rimcopy.wait_send()
    for k in range(1, nt):
        rcopy(k).wait_send()


def local(nz, ny, nt, tokens, norm_gain, pool_input, query_weight, key_weight, value_weight,
          pool_map, pool_scale, head_gain, diff_lambda, out_pool, out_heads):
    rows = tokens.shape[1]
    tables = [jnp.asarray(table) for table in rope_tables(rows, nz)]
    vmem = pl.BlockSpec(memory_space=pltpu.VMEM)
    anywhere = pl.BlockSpec(memory_space=pl.ANY)
    smem = pl.BlockSpec(memory_space=pltpu.SMEM)
    dma = pltpu.SemaphoreType.DMA
    far = nz // 2
    result = pl.pallas_call(
        functools.partial(kernel, nz, ny, nt),
        out_shape=jax.ShapeDtypeStruct((rows, 256), BF16),
        in_specs=[vmem, vmem, anywhere, anywhere, anywhere, anywhere, vmem, vmem, vmem, smem, vmem, vmem]
        + [vmem] * 4,
        out_specs=vmem,
        scratch_shapes=[
            pltpu.VMEM((rows, 2048), BF16),
            pltpu.VMEM((2048, 512), BF16),
            pltpu.VMEM((2048, 512), BF16),
            pltpu.VMEM((2048, 512), BF16),
            pltpu.VMEM((nz * rows, 512), BF16),
            pltpu.VMEM((rows, 256), BF16),
            pltpu.VMEM((rows, 256), BF16),
            pltpu.VMEM((16, 256), BF16),
            pltpu.VMEM((rows, 512), BF16),
            pltpu.VMEM((nt, rows, 256), BF16),
            pltpu.VMEM((nt, rows, 256), BF16),
            pltpu.VMEM((2, rows, 1), F32),
            pltpu.VMEM((2, rows, 1), F32),
            pltpu.VMEM((2, rows, 256), F32),
            dma((4,)),
            dma((3, 2, far)),
            dma((3, 2, far)),
            dma((3,)),
            dma((3, nz)),
            dma((3, nz)),
            dma((3, 2)),
            dma((2, far, 2)),
            dma((2, far, 2)),
            dma((2,)),
            dma((nt,)),
            dma((nt,)),
        ],
        compiler_params=pltpu.CompilerParams(
            collective_id=0, has_side_effects=True, vmem_limit_bytes=60 * 1024 * 1024
        ),
        name="layer",
    )(
        tokens[0], norm_gain.reshape(1, -1), pool_input, query_weight, key_weight, value_weight,
        pool_map, pool_scale.reshape(1, -1), head_gain.reshape(1, -1), diff_lambda, out_pool, out_heads,
        *tables,
    )
    return result[None]


def solution(mesh):
    placed = (
        P("fs", "sp", None),
        P(),
        P(("sp", "fs"), "tp"),
        P(("sp", "fs"), "tp"),
        P(("sp", "fs"), "tp"),
        P(("sp", "fs"), "tp"),
        P("tp", None, None),
        P("tp"),
        P(),
        P(),
        P("tp", ("sp", "fs")),
        P("tp", ("sp", "fs")),
    )
    sizes = (mesh.shape["sp"], mesh.shape["fs"], mesh.shape["tp"])
    return jax.shard_map(
        functools.partial(local, *sizes), mesh=mesh, in_specs=placed,
        out_specs=P("fs", "sp", "tp"), check_vma=False,
    )
```

```python
import functools

import numpy as np
import jax
import jax.numpy as jnp
from jax import lax
from jax.experimental import pallas as pl
from jax.experimental.pallas import tpu as pltpu
from jax.sharding import PartitionSpec as P

HEAD_DIM = 128
THETA = 500000.0
HEAD_SCALE = 0.8
NORM_EPS = 1e-06
HEAD_EPS = 1e-05
NEG = -1e30
F32 = jnp.float32
BF16 = jnp.bfloat16
MESH = pl.DeviceIdType.MESH
LOG2E = 1.4426950408889634


def rope_tables(rows, blocks):
    half = HEAD_DIM // 2
    freqs = 1.0 / THETA ** (np.arange(half, dtype=np.float64) * 2.0 / HEAD_DIM)
    tables = []
    for offsets in (np.arange(rows), np.arange(blocks) * rows):
        angles = offsets[:, None] * freqs[None, :]
        cosine, sine = np.cos(angles), np.sin(angles)
        tables.append(np.concatenate([cosine, cosine], 1).astype(np.float32))
        tables.append(np.concatenate([sine, sine], 1).astype(np.float32))
    return tables


def remote(src, dst, send, recv, **where):
    return pltpu.make_async_remote_copy(
        src_ref=src, dst_ref=dst, send_sem=send, recv_sem=recv, device_id=where, device_id_type=MESH
    )


def nt_dot(a, b):
    return lax.dot_general(a, b, (((1,), (1,)), ((), ())), preferred_element_type=F32)


def kernel(
    nz, ny, nt,
    tok_in, gain_in, pin, qw, kw, vw, pmap_in, pscale_in, hgain_in, lam_in, opool, ohead,
    rowcos_in, rowsin_in, blkcos_in, blksin_in,
    out,
    tok, gain, pmap, pscale, hgain, lam, rowcos, rowsin, blkcos, blksin,
    nrm, wkv, wqp, wo, kv, qbuf, poolbuf, rim, bra, part, rs,
    m_ref, l_ref, acc, mate, opp_in, side_in, opp_out,
    loc_sem, zsend, zrecv, ysend, yleft, yright, yopp, ksend, krecv, rimsem, dsend, drecv, matesend, materecv, rssend, rsrecv,
):
    z = lax.axis_index("sp")
    y = lax.axis_index("fs")
    t = lax.axis_index("tp")
    zr1 = lax.rem(z + 1, nz)
    zl1 = lax.rem(z + nz - 1, nz)
    yr1 = lax.rem(y + 1, ny)
    yl1 = lax.rem(y + ny - 1, ny)
    y2 = lax.rem(y + 2, ny)
    zr2 = lax.rem(z + 2, nz)
    zl2 = lax.rem(z + nz - 2, nz)
    rows = tok.shape[0]
    far = nz // 2
    groups = (wkv, wqp, wo)

    def slot(zz, yy):
        return pl.ds(pl.multiple_of(zz * 128 + yy * 32, 32), 32)

    own = slot(z, y)
    loads = [
        pltpu.make_async_copy(src, dst, loc_sem.at[i])
        for i, (src, dst) in enumerate((
            (kw, wkv.at[own, 0:256]),
            (vw, wkv.at[own, 256:512]),
            (pin, wqp.at[own, 0:256]),
            (qw, wqp.at[own, 256:512]),
            (opool, wo.at[own, 0:256]),
            (ohead, wo.at[own, 256:512]),
            (tok_in, tok),
            (gain_in, gain),
            (pmap_in, pmap),
            (pscale_in, pscale),
            (hgain_in, hgain),
            (lam_in, lam),
            (rowcos_in, rowcos),
            (rowsin_in, rowsin),
            (blkcos_in, blkcos),
            (blksin_in, blksin),
        ))
    ]
    for load in loads:
        load.start()

    barrier = pltpu.get_barrier_semaphore()
    friends = [{"sp": zr1}, {"sp": zl1}, {"sp": zr2}, {"sp": zl2}, {"fs": yr1}, {"fs": yl1}, {"fs": y2}]
    chip = t // 2
    side = lax.rem(t, 2)
    chips = nt // 2

    def device(away):
        return 2 * lax.rem(chip + away, chips) + side

    xr1, xl1, partner = device(1), device(chips - 1), 2 * chip + 1 - side
    friends += [{"tp": xr1}, {"tp": xl1}, {"tp": partner}]
    for where in friends:
        pl.semaphore_signal(barrier, inc=1, device_id=where, device_id_type=MESH)
    for load in loads[:6]:
        load.wait()
    pl.semaphore_wait(barrier, len(friends))

    def zslot(s, way):
        return lax.rem(z + nz - s, nz) if way == 0 else lax.rem(z + s, nz)

    def zcopy(g, way, s, stride=1):
        at = slot(zslot(s, way), y)
        peer = ((zr1, zl1), (zr2, zl2))[stride - 1][way]
        k = s + stride - 1
        return remote(
            groups[g].at[at], groups[g].at[at], zsend.at[g, way, k], zrecv.at[g, way, k], sp=peer
        )

    def zwait(g, way, s):
        at = slot(zslot(s, way), y)
        remote(
            groups[g].at[at], groups[g].at[at], zsend.at[g, way, s - 1], zrecv.at[g, way, s - 1], sp=zl1
        ).wait_recv()

    last = (far, nz - far - 1)

    def index_of(s, way):
        return 0 if s == 0 else 2 * s - 1 + way

    def steps_at(s):
        return [(s, way) for way in (0, 1) if s <= last[way] and not (s == 0 and way == 1)]

    def ysend_slots(g, s, way):
        buf = groups[g]
        at = slot(zslot(s, way), y)
        i = index_of(s, way)
        remote(buf.at[at], buf.at[at], ysend.at[g], yleft.at[g, i], fs=yr1).start()
        remote(buf.at[at], buf.at[at], ysend.at[g], yright.at[g, i], fs=yl1).start()

    def yrelay(g, s, way):
        buf = groups[g]
        zz = zslot(s, way)
        i = index_of(s, way)
        at = slot(zz, yl1)
        remote(buf.at[at], buf.at[at], ysend.at[g], yleft.at[g, i], fs=yr1).wait_recv()
        half = pl.ds(pl.multiple_of(zz * 128 + yl1 * 32, 16), 16)
        remote(buf.at[half], buf.at[half], ysend.at[g], yopp.at[g, 0], fs=yr1).start()
        at = slot(zz, yr1)
        remote(buf.at[at], buf.at[at], ysend.at[g], yright.at[g, i], fs=yl1).wait_recv()
        half = pl.ds(pl.multiple_of(zz * 128 + yr1 * 32 + 16, 16), 16)
        remote(buf.at[half], buf.at[half], ysend.at[g], yopp.at[g, 1], fs=yl1).start()

    direct = [pair for s in (far - 1, far) for pair in steps_at(s)]

    def yfar(step, way, i):
        at = slot(zslot(step, way), y)
        return remote(wkv.at[at], wkv.at[at], dsend.at[i], drecv.at[i], fs=y2)

    def yfinish(g):
        buf = groups[g]
        count = nz - (len(direct) if g == 0 else 0)
        for way in (0, 1):
            part_rows = buf.at[pl.ds(0, count * 16)]
            remote(part_rows, part_rows, ysend.at[g], yopp.at[g, way], fs=yr1).wait_recv()

    def lead(way, s):
        for stride in (2, 1):
            if s + stride <= last[way]:
                zcopy(0, way, s, stride).start()

    for way in (0, 1):
        lead(way, 0)
    ysend_slots(0, 0, 0)
    for g in (1, 2):
        for way in (0, 1):
            zcopy(g, way, 0).start()
    loads[6].wait()
    loads[7].wait()

    def norm_rows(i, carry):
        at = pl.ds(pl.multiple_of(i * 32, 32), 32)
        x = tok[at, :].astype(F32)
        scale = lax.rsqrt(jnp.mean(x * x, -1, keepdims=True) + NORM_EPS)
        nrm[at, :] = (x * scale * gain[...]).astype(BF16)
        return carry

    lax.fori_loop(0, rows // 32, norm_rows, 0)
    for load in loads[8:]:
        load.wait()

    def pass_on(s):
        for g in (1, 2):
            for step, way in steps_at(s):
                zwait(g, way, step)
                if step < last[way]:
                    zcopy(g, way, step).start()

    for k in range(1, far // 2 + 1):
        for way in (0, 1):
            if 2 * k <= last[way]:
                zwait(0, way, 2 * k)
                lead(way, 2 * k)
        for way in (0, 1):
            zwait(0, way, 2 * k - 1)
        fresh = steps_at(2 * k - 1) + steps_at(2 * k)
        for step, way in fresh:
            ysend_slots(0, step, way)
            if (step, way) in direct:
                yfar(step, way, direct.index((step, way))).start()
        earlier = [(0, 0)] if k == 1 else steps_at(2 * k - 3) + steps_at(2 * k - 2)
        for step, way in earlier:
            yrelay(0, step, way)
        pass_on(k)
    for i, (step, way) in enumerate(direct):
        at = slot(zslot(step, way), yl1)
        remote(wkv.at[at], wkv.at[at], ysend.at[0], yleft.at[0, index_of(step, way)], fs=yr1).wait_recv()
        at = slot(zslot(step, way), yr1)
        remote(wkv.at[at], wkv.at[at], ysend.at[0], yright.at[0, index_of(step, way)], fs=yl1).wait_recv()
        yfar(step, way, i).wait_recv()
    yfinish(0)
    cosine = rowcos[...] * blkcos[pl.ds(z, 1), :] - rowsin[...] * blksin[pl.ds(z, 1), :]
    sine = rowsin[...] * blkcos[pl.ds(z, 1), :] + rowcos[...] * blksin[pl.ds(z, 1), :]
    first = lax.broadcasted_iota(jnp.int32, sine.shape, 1) < HEAD_DIM // 2
    signed = jnp.where(first, -sine, sine)

    def rotated(x):
        x = x.astype(BF16).astype(F32)
        return (x * cosine + pltpu.roll(x, HEAD_DIM // 2, 1) * signed).astype(BF16)

    home = pl.ds(pl.multiple_of(z * rows, rows), rows)
    product = jnp.dot(nrm[...], wkv[:, 0:256], preferred_element_type=F32)
    kv[home, 0:128] = rotated(product[:, 0:128])
    kv[home, 128:256] = rotated(product[:, 128:256])
    kv[home, 256:512] = jnp.dot(nrm[...], wkv[:, 256:512], preferred_element_type=F32).astype(BF16)

    halfrows = rows // 2

    def kslot(s, way, half):
        zz = lax.rem(z + nz - s, nz) if way == 0 else lax.rem(z + s, nz)
        return pl.ds(pl.multiple_of(zz * rows + half * halfrows, halfrows), halfrows)

    def kcopy(s, way, half):
        at = kslot(s, way, half)
        return remote(
            kv.at[at], kv.at[at], ksend.at[way, s, half], krecv.at[way, s, half],
            sp=zr1 if way == 0 else zl1,
        )

    def kwait(s, way, half):
        at = kslot(s, way, half)
        remote(
            kv.at[at], kv.at[at], ksend.at[way, s - 1, half], krecv.at[way, s - 1, half], sp=zl1
        ).wait_recv()

    def halves(s, way):
        return (0, 1) if s < far else (way,)

    for half in (0, 1):
        for way in (0, 1):
            kcopy(0, way, half).start()

    order = [pair for s in range(far + 1) for pair in steps_at(s)]
    known = far // 2 + 1
    pass_on(known)
    for s in range(known + 1):
        for step, way in steps_at(s):
            ysend_slots(1, step, way)

    def ring(s):
        for half in (0, 1):
            for way in (0, 1):
                if half in halves(s, way):
                    kwait(s, way, half)
                    if s < far and half in halves(s + 1, way):
                        kcopy(s, way, half).start()

    for s in (1, 2, 3):
        ring(s)
        pass_on(known + s)
        for step, way in steps_at(known + s):
            ysend_slots(1, step, way)
        for step, way in order[(s - 1) * 4 : s * 4]:
            yrelay(1, step, way)
    ring(4)
    for step, way in order[12:]:
        yrelay(1, step, way)
    for step, way in order:
        ysend_slots(2, step, way)
    yfinish(1)
    product = jnp.dot(nrm[...], wqp[:, 256:512], preferred_element_type=F32)
    qbuf[:, 0:128] = rotated(product[:, 0:128])
    qbuf[:, 128:256] = rotated(product[:, 128:256])
    poolbuf[...] = jnp.dot(nrm[...], wqp[:, 0:256], preferred_element_type=F32).astype(BF16)
    rimcopy = remote(
        poolbuf.at[pl.ds(rows - 16, 16)], rim, rimsem.at[0], rimsem.at[1], sp=zr1
    )
    rimcopy.start()

    score_scale = HEAD_DIM ** (-0.5) * LOG2E

    def scores_of(j, m):
        at = pl.ds(pl.multiple_of(j * rows, rows), rows)
        cols = pl.ds(m * HEAD_DIM, HEAD_DIM)
        return nt_dot(qbuf[:, cols], kv[at, cols]) * score_scale

    def values_of(j):
        return kv[pl.ds(pl.multiple_of(j * rows, rows), rows), 256:512]

    for m in (0, 1):
        s0 = scores_of(z, m)
        above = lax.broadcasted_iota(jnp.int32, s0.shape, 1) > lax.broadcasted_iota(jnp.int32, s0.shape, 0)
        s0 = jnp.where(above, -jnp.inf, s0)
        top = jnp.max(s0, -1, keepdims=True)
        p = jnp.exp2(s0 - top)
        m_ref[m] = top
        l_ref[m] = jnp.sum(p, -1, keepdims=True)
        acc[m] = jnp.dot(p.astype(BF16), values_of(z), preferred_element_type=F32)

    def attend(j):
        for m in (0, 1):
            s0 = scores_of(j, m)
            old = m_ref[m]
            top = jnp.maximum(old, jnp.max(s0, -1, keepdims=True))
            p = jnp.exp2(s0 - top)
            shrink = jnp.exp2(old - top)
            m_ref[m] = top
            l_ref[m] = l_ref[m] * shrink + jnp.sum(p, -1, keepdims=True)
            acc[m] = acc[m] * shrink + jnp.dot(
                p.astype(BF16), values_of(j), preferred_element_type=F32
            )

    def attend_step(s):
        def one(way, carry):
            j = jnp.where(way == 0, z - s, z + s - nz)

            @pl.when(jnp.logical_and(j >= 0, s + way <= far))
            def _():
                attend(j)

            return carry

        lax.fori_loop(0, 2, one, 0)

    def backlog(s, carry):
        attend_step(s)
        return carry

    lax.fori_loop(1, 5, backlog, 0)

    for s in range(5, far + 1):
        ring(s)
        if s in (5, 6):
            for step, way in order[(s - 5) * 8 : (s - 4) * 8]:
                yrelay(2, step, way)
        if s == 5:
            rimcopy.wait_recv()
            level = lax.rem(t, 4)
            inner = poolbuf[...].astype(F32)
            before = jnp.where(z == 0, 0.0, rim[...].astype(F32))
            grown = jnp.concatenate([before, inner], 0)
            picked = jnp.zeros_like(grown)
            for power in range(4):
                grown = grown + pltpu.roll(grown, 1 << power, 0)
                picked = jnp.where(level == power, grown, picked)
            place = z * rows + lax.broadcasted_iota(jnp.int32, (rows, 1), 0)
            window = jnp.left_shift(2, level)
            count = jnp.minimum(place + 1, window).astype(F32)
            mixed = (picked[16:, :] / count - inner).astype(BF16)
            pooled = jnp.dot(mixed, pmap[0], preferred_element_type=F32) * pscale[...]
            bra[:, 0:256] = pooled.astype(BF16)
        attend_step(s)

    yfinish(2)
    here = lax.broadcasted_iota(jnp.int32, lam.shape, 1) == t
    weight = jnp.sum(jnp.where(here, lam[...], 0.0), -1, keepdims=True)
    heads = acc[0] / l_ref[0] - weight * (acc[1] / l_ref[1])
    scale = lax.rsqrt(jnp.mean(heads * heads, -1, keepdims=True) + HEAD_EPS)
    bra[:, 256:512] = (heads * scale * hgain[...] * HEAD_SCALE).astype(BF16)

    def partial_of(away, lane):
        block = 2 * lax.rem(chip + away, chips) + lane
        at = pl.ds(pl.multiple_of(block * 256, 256), 256)
        return nt_dot(bra[...], wo[at, :])

    def to_mate(i):
        return remote(part.at[i], mate.at[i], matesend.at[i], materecv.at[i], tp=partner)

    sequence = (2, 1, 3, 0)

    for i, away in enumerate(sequence):
        part[i] = partial_of(away, 1 - side).astype(BF16)
        to_mate(i).start()
    half_rows = rows // 2
    upper, lower = pl.ds(0, half_rows), pl.ds(half_rows, half_rows)
    own_sum = [partial_of(sequence[0], side)]
    to_mate(0).wait_recv()
    opp_out[...] = (own_sum[0] + mate[0].astype(F32)).astype(BF16)
    far_right = remote(opp_out.at[upper], opp_in.at[0], rssend.at[0], rsrecv.at[0], tp=xr1)
    far_left = remote(opp_out.at[lower], opp_in.at[1], rssend.at[1], rsrecv.at[1], tp=xl1)
    far_right.start()
    far_left.start()
    right_sum = partial_of(1, side)
    to_mate(1).wait_recv()
    right_sum = right_sum + mate[1].astype(F32)
    rs[0, lower, :] = right_sum[half_rows:].astype(BF16)
    near = [
        remote(rs.at[0, lower], side_in.at[0, lower], rssend.at[2], rsrecv.at[2], tp=xr1),
        remote(rs.at[1, upper], side_in.at[1, upper], rssend.at[3], rsrecv.at[3], tp=xl1),
        remote(rs.at[0, upper], side_in.at[0, upper], rssend.at[4], rsrecv.at[4], tp=xr1),
        remote(rs.at[1, lower], side_in.at[1, lower], rssend.at[5], rsrecv.at[5], tp=xl1),
    ]
    near[0].start()
    left_sum = partial_of(3, side)
    to_mate(2).wait_recv()
    left_sum = left_sum + mate[2].astype(F32)
    rs[1, upper, :] = left_sum[:half_rows].astype(BF16)
    near[1].start()
    total = partial_of(0, side)
    to_mate(3).wait_recv()
    total = total + mate[3].astype(F32)
    far_right.wait_recv()
    rs[0, upper, :] = (right_sum[:half_rows] + opp_in[0].astype(F32)).astype(BF16)
    near[2].start()
    far_left.wait_recv()
    rs[1, lower, :] = (left_sum[half_rows:] + opp_in[1].astype(F32)).astype(BF16)
    near[3].start()
    for copy in near:
        copy.wait_recv()
    out[...] = (total + side_in[0].astype(F32) + side_in[1].astype(F32)).astype(BF16)

    for g in range(3):
        for way in (0, 1):
            for k in range(1, last[way] + 1):
                at = slot(z, y)
                remote(
                    groups[g].at[at], groups[g].at[at], zsend.at[g, way, k - 1], zrecv.at[g, way, k - 1], sp=zl1
                ).wait_send()
        count = nz * 96 - (len(direct) * 32 if g == 0 else 0)
        whole = groups[g].at[pl.ds(0, count)]
        remote(whole, whole, ysend.at[g], yopp.at[g, 0], fs=yr1).wait_send()
    for i, (step, way) in enumerate(direct):
        yfar(step, way, i).wait_send()
    for way in (0, 1):
        for s in range(far):
            for half in halves(s + 1, way):
                kcopy(s, way, half).wait_send()
    rimcopy.wait_send()
    for i in range(4):
        to_mate(i).wait_send()
    for copy in [far_right, far_left] + near:
        copy.wait_send()


def local(nz, ny, nt, tokens, norm_gain, pool_input, query_weight, key_weight, value_weight,
          pool_map, pool_scale, head_gain, diff_lambda, out_pool, out_heads):
    rows = tokens.shape[1]
    tables = [jnp.asarray(table) for table in rope_tables(rows, nz)]
    vmem = pl.BlockSpec(memory_space=pltpu.VMEM)
    anywhere = pl.BlockSpec(memory_space=pl.ANY)
    dma = pltpu.SemaphoreType.DMA
    far = nz // 2
    result = pl.pallas_call(
        functools.partial(kernel, nz, ny, nt),
        out_shape=jax.ShapeDtypeStruct((rows, 256), BF16),
        in_specs=[anywhere] * 16,
        out_specs=vmem,
        scratch_shapes=[
            pltpu.VMEM((rows, 2048), BF16),
            pltpu.VMEM((1, 2048), F32),
            pltpu.VMEM((1, 256, 256), BF16),
            pltpu.VMEM((1, 256), F32),
            pltpu.VMEM((1, 256), F32),
            pltpu.VMEM((1, nt), F32),
            pltpu.VMEM((rows, HEAD_DIM), F32),
            pltpu.VMEM((rows, HEAD_DIM), F32),
            pltpu.VMEM((nz, HEAD_DIM), F32),
            pltpu.VMEM((nz, HEAD_DIM), F32),
            pltpu.VMEM((rows, 2048), BF16),
            pltpu.VMEM((2048, 512), BF16),
            pltpu.VMEM((2048, 512), BF16),
            pltpu.VMEM((2048, 512), BF16),
            pltpu.VMEM((nz * rows, 512), BF16),
            pltpu.VMEM((rows, 256), BF16),
            pltpu.VMEM((rows, 256), BF16),
            pltpu.VMEM((16, 256), BF16),
            pltpu.VMEM((rows, 512), BF16),
            pltpu.VMEM((4, rows, 256), BF16),
            pltpu.VMEM((2, rows, 256), BF16),
            pltpu.VMEM((2, rows, 1), F32),
            pltpu.VMEM((2, rows, 1), F32),
            pltpu.VMEM((2, rows, 256), F32),
            pltpu.VMEM((4, rows, 256), BF16),
            pltpu.VMEM((2, rows // 2, 256), BF16),
            pltpu.VMEM((2, rows, 256), BF16),
            pltpu.VMEM((rows, 256), BF16),
            dma((16,)),
            dma((3, 2, far)),
            dma((3, 2, far)),
            dma((3,)),
            dma((3, nz)),
            dma((3, nz)),
            dma((3, 2)),
            dma((2, far, 2)),
            dma((2, far, 2)),
            dma((2,)),
            dma((3,)),
            dma((3,)),
            dma((4,)),
            dma((4,)),
            dma((6,)),
            dma((6,)),
        ],
        compiler_params=pltpu.CompilerParams(
            collective_id=0, has_side_effects=True, vmem_limit_bytes=60 * 1024 * 1024
        ),
        name="layer",
    )(
        tokens[0], norm_gain.reshape(1, -1), pool_input, query_weight, key_weight, value_weight,
        pool_map, pool_scale.reshape(1, -1), head_gain.reshape(1, -1),
        diff_lambda.reshape(1, -1), out_pool.T, out_heads.T,
        *tables,
    )
    return result[None]


def solution(mesh):
    placed = (
        P("fs", "sp", None),
        P(),
        P(("sp", "fs"), "tp"),
        P(("sp", "fs"), "tp"),
        P(("sp", "fs"), "tp"),
        P(("sp", "fs"), "tp"),
        P("tp", None, None),
        P("tp"),
        P(),
        P(),
        P("tp", ("sp", "fs")),
        P("tp", ("sp", "fs")),
    )
    sizes = (mesh.shape["sp"], mesh.shape["fs"], mesh.shape["tp"])
    return jax.shard_map(
        functools.partial(local, *sizes), mesh=mesh, in_specs=placed,
        out_specs=P("fs", "sp", "tp"), check_vma=False,
    )
```

```python
import functools

import numpy as np
import jax
import jax.numpy as jnp
from jax import lax
from jax.experimental import pallas as pl
from jax.experimental.pallas import tpu as pltpu
from jax.sharding import PartitionSpec as P

HEAD_DIM = 128
THETA = 500000.0
HEAD_SCALE = 0.8
NORM_EPS = 1e-06
HEAD_EPS = 1e-05
NEG = -1e30
F32 = jnp.float32
BF16 = jnp.bfloat16
MESH = pl.DeviceIdType.MESH
LOG2E = 1.4426950408889634


def rope_tables(rows, blocks):
    half = HEAD_DIM // 2
    freqs = 1.0 / THETA ** (np.arange(half, dtype=np.float64) * 2.0 / HEAD_DIM)
    tables = []
    for offsets in (np.arange(rows), np.arange(blocks) * rows):
        angles = offsets[:, None] * freqs[None, :]
        cosine, sine = np.cos(angles), np.sin(angles)
        tables.append(np.concatenate([cosine, cosine], 1).astype(np.float32))
        tables.append(np.concatenate([sine, sine], 1).astype(np.float32))
    return tables


def remote(src, dst, send, recv, **where):
    return pltpu.make_async_remote_copy(
        src_ref=src, dst_ref=dst, send_sem=send, recv_sem=recv, device_id=where, device_id_type=MESH
    )


def nt_dot(a, b):
    return lax.dot_general(a, b, (((1,), (1,)), ((), ())), preferred_element_type=F32)


def kernel(
    nz, ny, nt,
    tok_in, gain_in, pin, qw, kw, vw, pmap_in, pscale_in, hgain_in, lam_in, opool, ohead,
    rowcos_in, rowsin_in, blkcos_in, blksin_in,
    out,
    tok, gain, pmap, pscale, hgain, lam, rowcos, rowsin, blkcos, blksin,
    nrm, wkv, wqp, wo, kv, qbuf, poolbuf, rim, bra, part, rs,
    m_ref, l_ref, acc, mate, opp_in, side_in, opp_out,
    loc_sem, zsend, zrecv, ysend, yleft, yright, yopp, ksend, krecv, rimsem, dsend, drecv, matesend, materecv, rssend, rsrecv,
):
    z = lax.axis_index("sp")
    y = lax.axis_index("fs")
    t = lax.axis_index("tp")
    zr1 = lax.rem(z + 1, nz)
    zl1 = lax.rem(z + nz - 1, nz)
    yr1 = lax.rem(y + 1, ny)
    yl1 = lax.rem(y + ny - 1, ny)
    y2 = lax.rem(y + 2, ny)
    zr2 = lax.rem(z + 2, nz)
    zl2 = lax.rem(z + nz - 2, nz)
    rows = tok.shape[0]
    far = nz // 2
    groups = (wkv, wqp, wo)

    def slot(zz, yy):
        return pl.ds(pl.multiple_of(zz * 128 + yy * 32, 32), 32)

    own = slot(z, y)
    loads = [
        pltpu.make_async_copy(src, dst, loc_sem.at[i])
        for i, (src, dst) in enumerate((
            (kw, wkv.at[own, 0:256]),
            (vw, wkv.at[own, 256:512]),
            (pin, wqp.at[own, 0:256]),
            (qw, wqp.at[own, 256:512]),
            (opool, wo.at[own, 0:256]),
            (ohead, wo.at[own, 256:512]),
            (tok_in, tok),
            (gain_in, gain),
            (pmap_in, pmap),
            (pscale_in, pscale),
            (hgain_in, hgain),
            (lam_in, lam),
            (rowcos_in, rowcos),
            (rowsin_in, rowsin),
            (blkcos_in, blkcos),
            (blksin_in, blksin),
        ))
    ]
    for load in loads:
        load.start()

    barrier = pltpu.get_barrier_semaphore()
    friends = [{"sp": zr1}, {"sp": zl1}, {"sp": zr2}, {"sp": zl2}, {"fs": yr1}, {"fs": yl1}, {"fs": y2}]
    chip = t // 2
    side = lax.rem(t, 2)
    chips = nt // 2

    def device(away):
        return 2 * lax.rem(chip + away, chips) + side

    xr1, xl1, partner = device(1), device(chips - 1), 2 * chip + 1 - side
    friends += [{"tp": xr1}, {"tp": xl1}, {"tp": partner}]
    for where in friends:
        pl.semaphore_signal(barrier, inc=1, device_id=where, device_id_type=MESH)
    for load in loads[:6]:
        load.wait()
    pl.semaphore_wait(barrier, len(friends))

    def zslot(s, way):
        return lax.rem(z + nz - s, nz) if way == 0 else lax.rem(z + s, nz)

    def zcopy(g, way, s, stride=1):
        at = slot(zslot(s, way), y)
        peer = ((zr1, zl1), (zr2, zl2))[stride - 1][way]
        k = s + stride - 1
        return remote(
            groups[g].at[at], groups[g].at[at], zsend.at[g, way, k], zrecv.at[g, way, k], sp=peer
        )

    def zwait(g, way, s):
        at = slot(zslot(s, way), y)
        remote(
            groups[g].at[at], groups[g].at[at], zsend.at[g, way, s - 1], zrecv.at[g, way, s - 1], sp=zl1
        ).wait_recv()

    last = (far, nz - far - 1)

    def index_of(s, way):
        return 0 if s == 0 else 2 * s - 1 + way

    def steps_at(s):
        return [(s, way) for way in (0, 1) if s <= last[way] and not (s == 0 and way == 1)]

    def ysend_slots(g, s, way):
        buf = groups[g]
        at = slot(zslot(s, way), y)
        i = index_of(s, way)
        remote(buf.at[at], buf.at[at], ysend.at[g], yleft.at[g, i], fs=yr1).start()
        remote(buf.at[at], buf.at[at], ysend.at[g], yright.at[g, i], fs=yl1).start()

    def yrelay(g, s, way):
        buf = groups[g]
        zz = zslot(s, way)
        i = index_of(s, way)
        at = slot(zz, yl1)
        remote(buf.at[at], buf.at[at], ysend.at[g], yleft.at[g, i], fs=yr1).wait_recv()
        half = pl.ds(pl.multiple_of(zz * 128 + yl1 * 32, 16), 16)
        remote(buf.at[half], buf.at[half], ysend.at[g], yopp.at[g, 0], fs=yr1).start()
        at = slot(zz, yr1)
        remote(buf.at[at], buf.at[at], ysend.at[g], yright.at[g, i], fs=yl1).wait_recv()
        half = pl.ds(pl.multiple_of(zz * 128 + yr1 * 32 + 16, 16), 16)
        remote(buf.at[half], buf.at[half], ysend.at[g], yopp.at[g, 1], fs=yl1).start()

    direct = [pair for s in (far - 1, far) for pair in steps_at(s)]

    def yfar(step, way, i):
        at = slot(zslot(step, way), y)
        return remote(wkv.at[at], wkv.at[at], dsend.at[i], drecv.at[i], fs=y2)

    def yfinish(g):
        buf = groups[g]
        count = nz - (len(direct) if g == 0 else 0)
        for way in (0, 1):
            part_rows = buf.at[pl.ds(0, count * 16)]
            remote(part_rows, part_rows, ysend.at[g], yopp.at[g, way], fs=yr1).wait_recv()

    def lead(way, s):
        for stride in (2, 1):
            if s + stride <= last[way]:
                zcopy(0, way, s, stride).start()

    for way in (0, 1):
        lead(way, 0)
    ysend_slots(0, 0, 0)
    for g in (1, 2):
        for way in (0, 1):
            zcopy(g, way, 0).start()
    loads[6].wait()
    loads[7].wait()

    def norm_rows(i, carry):
        at = pl.ds(pl.multiple_of(i * 32, 32), 32)
        x = tok[at, :].astype(F32)
        scale = lax.rsqrt(jnp.mean(x * x, -1, keepdims=True) + NORM_EPS)
        nrm[at, :] = (x * scale * gain[...]).astype(BF16)
        return carry

    lax.fori_loop(0, rows // 32, norm_rows, 0)
    for load in loads[8:]:
        load.wait()

    def pass_on(s):
        for g in (1, 2):
            for step, way in steps_at(s):
                zwait(g, way, step)
                if step < last[way]:
                    zcopy(g, way, step).start()

    for k in range(1, far // 2 + 1):
        for way in (0, 1):
            if 2 * k <= last[way]:
                zwait(0, way, 2 * k)
                lead(way, 2 * k)
        for way in (0, 1):
            zwait(0, way, 2 * k - 1)
        fresh = steps_at(2 * k - 1) + steps_at(2 * k)
        for step, way in fresh:
            ysend_slots(0, step, way)
            if (step, way) in direct:
                yfar(step, way, direct.index((step, way))).start()
        earlier = [(0, 0)] if k == 1 else steps_at(2 * k - 3) + steps_at(2 * k - 2)
        for step, way in earlier:
            yrelay(0, step, way)
        pass_on(k)
    pass_on(far // 2 + 1)
    for i, (step, way) in enumerate(direct):
        at = slot(zslot(step, way), yl1)
        remote(wkv.at[at], wkv.at[at], ysend.at[0], yleft.at[0, index_of(step, way)], fs=yr1).wait_recv()
        at = slot(zslot(step, way), yr1)
        remote(wkv.at[at], wkv.at[at], ysend.at[0], yright.at[0, index_of(step, way)], fs=yl1).wait_recv()
        yfar(step, way, i).wait_recv()
    yfinish(0)
    pass_on(far // 2 + 2)
    cosine = rowcos[...] * blkcos[pl.ds(z, 1), :] - rowsin[...] * blksin[pl.ds(z, 1), :]
    sine = rowsin[...] * blkcos[pl.ds(z, 1), :] + rowcos[...] * blksin[pl.ds(z, 1), :]
    first = lax.broadcasted_iota(jnp.int32, sine.shape, 1) < HEAD_DIM // 2
    signed = jnp.where(first, -sine, sine)

    def rotated(x):
        x = x.astype(BF16).astype(F32)
        return (x * cosine + pltpu.roll(x, HEAD_DIM // 2, 1) * signed).astype(BF16)

    home = pl.ds(pl.multiple_of(z * rows, rows), rows)
    product = jnp.dot(nrm[...], wkv[:, 0:256], preferred_element_type=F32)
    kv[home, 0:128] = rotated(product[:, 0:128])
    kv[home, 128:256] = rotated(product[:, 128:256])
    kv[home, 256:512] = jnp.dot(nrm[...], wkv[:, 256:512], preferred_element_type=F32).astype(BF16)

    pieces = 4
    span = rows // pieces

    def kslot(s, way, c):
        return pl.ds(pl.multiple_of(zslot(s, way) * rows + c * span, span), span)

    def kcopy(s, way, c):
        at = kslot(s, way, c)
        return remote(
            kv.at[at], kv.at[at], ksend.at[way, s, c], krecv.at[way, s, c],
            sp=zr1 if way == 0 else zl1,
        )

    def kwait(s, way, c):
        at = kslot(s, way, c)
        remote(
            kv.at[at], kv.at[at], ksend.at[way, s - 1, c], krecv.at[way, s - 1, c], sp=zl1
        ).wait_recv()

    def service(s, c):
        for way in (0, 1):
            kwait(s, way, c)
            kept = c < pieces // 2 if way == 0 else c >= pieces // 2

            @pl.when(jnp.logical_or(s < far - 1, kept))
            def _():
                kcopy(s, way, c).start()

    for c in range(pieces):
        for way in (0, 1):
            kcopy(0, way, c).start()

    order = [pair for s in range(far + 1) for pair in steps_at(s)]
    known = far // 2 + 2
    for s in range(known + 1):
        for step, way in steps_at(s):
            ysend_slots(1, step, way)

    for s in (1, 2, 3):
        for c in range(pieces):
            service(s, c)
            if c == 1 and known + s <= far:
                pass_on(known + s)
                for step, way in steps_at(known + s):
                    ysend_slots(1, step, way)
            at = (s - 1) * pieces + c
            for step, way in order[at : at + 1] if at < 8 else order[8 + 2 * (at - 8) : 10 + 2 * (at - 8)]:
                yrelay(1, step, way)
    for step, way in order:
        ysend_slots(2, step, way)
    yfinish(1)
    product = jnp.dot(nrm[...], wqp[:, 256:512], preferred_element_type=F32)
    qbuf[:, 0:128] = rotated(product[:, 0:128])
    qbuf[:, 128:256] = rotated(product[:, 128:256])
    poolbuf[...] = jnp.dot(nrm[...], wqp[:, 0:256], preferred_element_type=F32).astype(BF16)
    rimcopy = remote(
        poolbuf.at[pl.ds(rows - 16, 16)], rim, rimsem.at[0], rimsem.at[1], sp=zr1
    )
    rimcopy.start()

    score_scale = HEAD_DIM ** (-0.5) * LOG2E

    def scores_of(j, m):
        at = pl.ds(pl.multiple_of(j * rows, rows), rows)
        cols = pl.ds(m * HEAD_DIM, HEAD_DIM)
        return nt_dot(qbuf[:, cols], kv[at, cols]) * score_scale

    def values_of(j):
        return kv[pl.ds(pl.multiple_of(j * rows, rows), rows), 256:512]

    m_ref[...] = jnp.full(m_ref.shape, NEG, F32)
    l_ref[...] = jnp.zeros(l_ref.shape, F32)
    acc[...] = jnp.zeros(acc.shape, F32)
    above = lax.broadcasted_iota(jnp.int32, (rows, rows), 1) > lax.broadcasted_iota(jnp.int32, (rows, rows), 0)

    def attend(n):
        step = (n + 1) // 2
        way = lax.rem(n + 1, 2)
        j = jnp.where(n == 0, z, jnp.where(way == 0, z - step, z + step - nz))

        @pl.when(j >= 0)
        def _():
            for m in (0, 1):
                s0 = scores_of(j, m)
                s0 = jnp.where(jnp.logical_and(above, j == z), -jnp.inf, s0)
                old = m_ref[m]
                top = jnp.maximum(old, jnp.max(s0, -1, keepdims=True))
                p = jnp.exp2(s0 - top)
                shrink = jnp.exp2(old - top)
                m_ref[m] = top
                l_ref[m] = l_ref[m] * shrink + jnp.sum(p, -1, keepdims=True)
                acc[m] = acc[m] * shrink + jnp.dot(
                    p.astype(BF16), values_of(j), preferred_element_type=F32
                )

    def zplace(n):
        step = (n + 1) // 2
        return jnp.where(lax.rem(n + 1, 2) == 0, lax.rem(z + nz - step, nz), lax.rem(z + step, nz))

    def orelay(n):
        zz = zplace(n)
        at = slot(zz, yl1)
        remote(wo.at[at], wo.at[at], ysend.at[2], yleft.at[2, n], fs=yr1).wait_recv()
        half = pl.ds(pl.multiple_of(zz * 128 + yl1 * 32, 16), 16)
        remote(wo.at[half], wo.at[half], ysend.at[2], yopp.at[2, 0], fs=yr1).start()
        at = slot(zz, yr1)
        remote(wo.at[at], wo.at[at], ysend.at[2], yright.at[2, n], fs=yl1).wait_recv()
        half = pl.ds(pl.multiple_of(zz * 128 + yr1 * 32 + 16, 16), 16)
        remote(wo.at[half], wo.at[half], ysend.at[2], yopp.at[2, 1], fs=yl1).start()

    def busy(i, carry):
        s, c = 4 + i // pieces, lax.rem(i, pieces)
        service(s, c)
        orelay(i)

        @pl.when(c < 3)
        def _():
            attend(3 * (s - 4) + c)

        return carry

    lax.fori_loop(0, 4 * pieces, busy, 0)
    rimcopy.wait_recv()
    level = lax.rem(t, 4)
    inner = poolbuf[...].astype(F32)
    before = jnp.where(z == 0, 0.0, rim[...].astype(F32))
    grown = jnp.concatenate([before, inner], 0)
    picked = jnp.zeros_like(grown)
    for power in range(4):
        grown = grown + pltpu.roll(grown, 1 << power, 0)
        picked = jnp.where(level == power, grown, picked)
    place = z * rows + lax.broadcasted_iota(jnp.int32, (rows, 1), 0)
    window = jnp.left_shift(2, level)
    count = jnp.minimum(place + 1, window).astype(F32)
    mixed = (picked[16:, :] / count - inner).astype(BF16)
    pooled = jnp.dot(mixed, pmap[0], preferred_element_type=F32) * pscale[...]
    bra[:, 0:256] = pooled.astype(BF16)

    def late(n, carry):
        attend(n)
        return carry

    lax.fori_loop(12, 15, late, 0)
    for c in range(pieces // 2):
        kwait(far, 0, c)
        kwait(far, 1, c + pieces // 2)
    lax.fori_loop(15, 16, late, 0)
    yfinish(2)
    here = lax.broadcasted_iota(jnp.int32, lam.shape, 1) == t
    weight = jnp.sum(jnp.where(here, lam[...], 0.0), -1, keepdims=True)
    heads = acc[0] / l_ref[0] - weight * (acc[1] / l_ref[1])
    scale = lax.rsqrt(jnp.mean(heads * heads, -1, keepdims=True) + HEAD_EPS)
    bra[:, 256:512] = (heads * scale * hgain[...] * HEAD_SCALE).astype(BF16)

    def partial_of(away, lane):
        block = 2 * lax.rem(chip + away, chips) + lane
        at = pl.ds(pl.multiple_of(block * 256, 256), 256)
        return nt_dot(bra[...], wo[at, :])

    def to_mate(i):
        return remote(part.at[i], mate.at[i], matesend.at[i], materecv.at[i], tp=partner)

    sequence = (2, 1, 3, 0)

    for i, away in enumerate(sequence):
        part[i] = partial_of(away, 1 - side).astype(BF16)
        to_mate(i).start()
    half_rows = rows // 2
    upper, lower = pl.ds(0, half_rows), pl.ds(half_rows, half_rows)
    own_sum = [partial_of(sequence[0], side)]
    to_mate(0).wait_recv()
    opp_out[...] = (own_sum[0] + mate[0].astype(F32)).astype(BF16)
    far_right = remote(opp_out.at[upper], opp_in.at[0], rssend.at[0], rsrecv.at[0], tp=xr1)
    far_left = remote(opp_out.at[lower], opp_in.at[1], rssend.at[1], rsrecv.at[1], tp=xl1)
    far_right.start()
    far_left.start()
    right_sum = partial_of(1, side)
    to_mate(1).wait_recv()
    right_sum = right_sum + mate[1].astype(F32)
    rs[0, lower, :] = right_sum[half_rows:].astype(BF16)
    near = [
        remote(rs.at[0, lower], side_in.at[0, lower], rssend.at[2], rsrecv.at[2], tp=xr1),
        remote(rs.at[1, upper], side_in.at[1, upper], rssend.at[3], rsrecv.at[3], tp=xl1),
        remote(rs.at[0, upper], side_in.at[0, upper], rssend.at[4], rsrecv.at[4], tp=xr1),
        remote(rs.at[1, lower], side_in.at[1, lower], rssend.at[5], rsrecv.at[5], tp=xl1),
    ]
    near[0].start()
    left_sum = partial_of(3, side)
    to_mate(2).wait_recv()
    left_sum = left_sum + mate[2].astype(F32)
    rs[1, upper, :] = left_sum[:half_rows].astype(BF16)
    near[1].start()
    total = partial_of(0, side)
    to_mate(3).wait_recv()
    total = total + mate[3].astype(F32)
    far_right.wait_recv()
    rs[0, upper, :] = (right_sum[:half_rows] + opp_in[0].astype(F32)).astype(BF16)
    near[2].start()
    far_left.wait_recv()
    rs[1, lower, :] = (left_sum[half_rows:] + opp_in[1].astype(F32)).astype(BF16)
    near[3].start()
    for copy in near:
        copy.wait_recv()
    out[...] = (total + side_in[0].astype(F32) + side_in[1].astype(F32)).astype(BF16)

    for g in range(3):
        for way in (0, 1):
            for k in range(1, last[way] + 1):
                at = slot(z, y)
                remote(
                    groups[g].at[at], groups[g].at[at], zsend.at[g, way, k - 1], zrecv.at[g, way, k - 1], sp=zl1
                ).wait_send()
        count = nz * 96 - (len(direct) * 32 if g == 0 else 0)
        whole = groups[g].at[pl.ds(0, count)]
        remote(whole, whole, ysend.at[g], yopp.at[g, 0], fs=yr1).wait_send()
    for i, (step, way) in enumerate(direct):
        yfar(step, way, i).wait_send()
    for way in (0, 1):
        for s in range(far):
            for c in range(pieces):
                if s < far - 1 or c // (pieces // 2) == way:
                    kcopy(s, way, c).wait_send()
    rimcopy.wait_send()
    for i in range(4):
        to_mate(i).wait_send()
    for copy in [far_right, far_left] + near:
        copy.wait_send()


def local(nz, ny, nt, tokens, norm_gain, pool_input, query_weight, key_weight, value_weight,
          pool_map, pool_scale, head_gain, diff_lambda, out_pool, out_heads):
    rows = tokens.shape[1]
    tables = [jnp.asarray(table) for table in rope_tables(rows, nz)]
    vmem = pl.BlockSpec(memory_space=pltpu.VMEM)
    anywhere = pl.BlockSpec(memory_space=pl.ANY)
    dma = pltpu.SemaphoreType.DMA
    far = nz // 2
    result = pl.pallas_call(
        functools.partial(kernel, nz, ny, nt),
        out_shape=jax.ShapeDtypeStruct((rows, 256), BF16),
        in_specs=[anywhere] * 16,
        out_specs=vmem,
        scratch_shapes=[
            pltpu.VMEM((rows, 2048), BF16),
            pltpu.VMEM((1, 2048), F32),
            pltpu.VMEM((1, 256, 256), BF16),
            pltpu.VMEM((1, 256), F32),
            pltpu.VMEM((1, 256), F32),
            pltpu.VMEM((1, nt), F32),
            pltpu.VMEM((rows, HEAD_DIM), F32),
            pltpu.VMEM((rows, HEAD_DIM), F32),
            pltpu.VMEM((nz, HEAD_DIM), F32),
            pltpu.VMEM((nz, HEAD_DIM), F32),
            pltpu.VMEM((rows, 2048), BF16),
            pltpu.VMEM((2048, 512), BF16),
            pltpu.VMEM((2048, 512), BF16),
            pltpu.VMEM((2048, 512), BF16),
            pltpu.VMEM((nz * rows, 512), BF16),
            pltpu.VMEM((rows, 256), BF16),
            pltpu.VMEM((rows, 256), BF16),
            pltpu.VMEM((16, 256), BF16),
            pltpu.VMEM((rows, 512), BF16),
            pltpu.VMEM((4, rows, 256), BF16),
            pltpu.VMEM((2, rows, 256), BF16),
            pltpu.VMEM((2, rows, 1), F32),
            pltpu.VMEM((2, rows, 1), F32),
            pltpu.VMEM((2, rows, 256), F32),
            pltpu.VMEM((4, rows, 256), BF16),
            pltpu.VMEM((2, rows // 2, 256), BF16),
            pltpu.VMEM((2, rows, 256), BF16),
            pltpu.VMEM((rows, 256), BF16),
            dma((16,)),
            dma((3, 2, far)),
            dma((3, 2, far)),
            dma((3,)),
            dma((3, nz)),
            dma((3, nz)),
            dma((3, 2)),
            dma((2, far, 4)),
            dma((2, far, 4)),
            dma((2,)),
            dma((3,)),
            dma((3,)),
            dma((4,)),
            dma((4,)),
            dma((6,)),
            dma((6,)),
        ],
        compiler_params=pltpu.CompilerParams(
            collective_id=0, has_side_effects=True, vmem_limit_bytes=60 * 1024 * 1024
        ),
        name="layer",
    )(
        tokens[0], norm_gain.reshape(1, -1), pool_input, query_weight, key_weight, value_weight,
        pool_map, pool_scale.reshape(1, -1), head_gain.reshape(1, -1),
        diff_lambda.reshape(1, -1), out_pool.T, out_heads.T,
        *tables,
    )
    return result[None]


def solution(mesh):
    placed = (
        P("fs", "sp", None),
        P(),
        P(("sp", "fs"), "tp"),
        P(("sp", "fs"), "tp"),
        P(("sp", "fs"), "tp"),
        P(("sp", "fs"), "tp"),
        P("tp", None, None),
        P("tp"),
        P(),
        P(),
        P("tp", ("sp", "fs")),
        P("tp", ("sp", "fs")),
    )
    sizes = (mesh.shape["sp"], mesh.shape["fs"], mesh.shape["tp"])
    return jax.shard_map(
        functools.partial(local, *sizes), mesh=mesh, in_specs=placed,
        out_specs=P("fs", "sp", "tp"), check_vma=False,
    )
```
